128 devices in a mesh: grp: 4 (over y, x), ep: 32 (over z, core).
Axes of the slice: x: 2, y: 2, z: 16, core: 2. Of those that a mesh axis runs over, the one named last changes fastest.
The devices are a block of a 8x8x16 slice.
Arguments:
- tokens: bfloat16 [4096, 2048], P(('grp', 'ep')), parts along dimension 0, may hold values from -6 to 6
- routes: int32 [4096, 4], P(('grp', 'ep')), parts along dimension 0, may hold values from 0 to 31, all different within a row; in each aligned block of 32 rows (0 to 31, 32 to 63, ...) at most 8 rows name the same one
- route_logits: float32 [4096, 4], P(('grp', 'ep')), parts along dimension 0, may hold values from -4 to 4
- state_real: float32 [4096, 64, 64], P('grp', 'ep'), parts along dimension 0, may hold values from -4 to 4
- state_imag: float32 [4096, 64, 64], P('grp', 'ep'), parts along dimension 0, may hold values from -4 to 4
- gain_in: float32 [2048], replicated, may hold values from 0.1 to 1.9
- proj_in: bfloat16 [2048, 1024], P(None, 'ep'), may hold values from -0.125 to 0.125
- decay_rate: float32 [64, 64], P('ep'), may hold values from 0.05 to 2
- frequency: float32 [64, 64], P('ep'), may hold values from -4 to 4
- log_step: float32 [64], P('ep'), may hold values from -3 to 0
- input_real: float32 [64, 64, 16], P('ep'), may hold values from -1 to 1
- input_imag: float32 [64, 64, 16], P('ep'), may hold values from -1 to 1
- output_real: float32 [64, 16, 64], P('ep'), may hold values from -0.5 to 0.5
- output_imag: float32 [64, 16, 64], P('ep'), may hold values from -0.5 to 0.5
- skip_gain: float32 [64, 16], P('ep'), may hold values from -4 to 4
- proj_out: bfloat16 [1024, 2048], P('ep'), may hold values from -0.1875 to 0.1875
- gain_mid: float32 [2048], replicated, may hold values from 0.1 to 1.9
- expert_gate: bfloat16 [32, 2048, 1024], P('ep'), may hold values from -0.33007812 to 0.33007812
- expert_up: bfloat16 [32, 2048, 1024], P('ep'), may hold values from -0.33007812 to 0.33007812
- expert_down: bfloat16 [32, 1024, 2048], P('ep'), may hold values from -0.056152344 to 0.056152344
- dense_gate: bfloat16 [2048, 2048], P(None, 'ep'), may hold values from -0.125 to 0.125
- dense_up: bfloat16 [2048, 2048], P(None, 'ep'), may hold values from -0.125 to 0.125
- dense_down: bfloat16 [2048, 2048], P('ep'), may hold values from -0.125 to 0.125
- dense_mix: float32 [2048], P('ep'), may hold values from -0.39774758 to 0.39774758
Outputs:
- layer_out: bfloat16 [4096, 2048], P(('grp', 'ep')), parts along dimension 0
- state_real_new: float32 [4096, 64, 64], P('grp', 'ep'), parts along dimension 0
- state_imag_new: float32 [4096, 64, 64], P('grp', 'ep'), parts along dimension 0
The draws below stay inside these ranges and needn't reach their ends.
There are 4 independent parts, one for each index of `grp`. The reference program is written for one: setup_inputs(seed, part) draws one part's arguments, and reference() takes and returns one part's arrays. A program takes and returns all parts, laid end to end along the dimension named above; an argument that names none is the same for every part. Nothing has to cross between parts.
Inputs may be any that keep to these rules, and one draw needn't show every extreme that they name: `routes`: each row names 4 different experts; among the rows of one device no expert is named more than 8 times, and in every draw some device names some expert exactly 8 times.
All inputs are finite; a program needn't handle non-finite values.
Results may differ from the reference program's by a relative error of at most 0.015.
Values may be sent and summed in bfloat16 or wider, within the bound.
No kernel may reach another device: no remote copies, remote signals or barrier semaphores. Data moves between devices by JAX's collectives and lax.ppermute only.
A program may use at most 128 MiB of HBM per device.

```python
import math
import jax
import jax.numpy as jnp
import numpy as np
from jax import lax

D = 2048
CHANNELS = 1024
GROUP = 16
GROUPS = 64
STATE = 64
FF = 1024
DENSE = 2048
TOPK = 4
EXPERTS = 32
SEQ_DEV = 32
SEQS = 1024
CAP = 8
N_EP = 32


def block_scale(key, shape, split, smallest, top_value):
    def one(axis_at, parts):
        steps = jax.random.uniform(jax.random.fold_in(jax.random.fold_in(key, 6), axis_at), (parts,), jnp.float32, smallest / len(split), top_value / len(split))
        return jnp.repeat(jnp.exp(steps), shape[axis_at] // parts).reshape((-1,) + (1,) * (len(shape) - axis_at - 1))

    gain = one(*split[0])
    for cut in split[1:]:
        gain = gain * one(*cut)
    return gain


def assign_block(key, own, number, rows, count, top, most, slope):
    sequence = jax.random.permutation(key, count)
    heavy_load, ordinary = load_shares(count, rows * top, most, slope, True), load_shares(count, rows * top, most, slope, False)
    places = jnp.arange(count)

    def named(lengths, rotation):
        used = int((lengths > 0).sum())
        fixed = max(1, used // 4)
        moved = fixed + (places - fixed + rotation * (used - fixed)) % max(1, count - fixed)
        return jnp.zeros((count,), jnp.int32).at[sequence[jnp.where(places < fixed, places, moved)]].set(jnp.asarray(lengths, jnp.int32))

    lengths = jnp.where(number % 4 == 0, named(heavy_load, number // 4), named(ordinary, number - number // 4 - 1))
    mixed = jax.random.permutation(jax.random.fold_in(own, 3), count)
    source_of, taker = mixed[0:count // 2 * 2:2], mixed[1:count // 2 * 2:2]
    slack = jnp.minimum(lengths[source_of] - 1, most - lengths[taker]) // 2
    slack = jnp.where((source_of == sequence[0]) | (taker == sequence[0]) | (lengths[taker] == 0), 0, jnp.maximum(slack, 0))
    moved = jax.random.randint(jax.random.fold_in(own, 4), (count // 2,), 0, 1 << 20) % (slack + 1)
    lengths = lengths.at[source_of].add(-moved).at[taker].add(moved)
    labels = jnp.searchsorted(jnp.cumsum(lengths), jnp.arange(rows * top), side="right").astype(jnp.int32)
    table = labels.reshape(top, rows).T
    table = table[jax.random.permutation(jax.random.fold_in(own, 1), rows)]
    rotation = jax.random.randint(jax.random.fold_in(own, 2), (rows, 1), 0, top)
    return jnp.take_along_axis(table, (jnp.arange(top)[None, :] + rotation) % top, axis=1)


def load_shares(amount, total, limit, skew, full):
    loads = [(1 << 20) // math.isqrt(grade ** skew) + 1 for grade in range(1, amount + 1)]
    largest = limit if full else min(limit, max(-(-total // amount), total * loads[0] // sum(loads)))
    least = 1 if total - largest >= amount - 1 else 0
    given, rest = [largest] + [least] * (amount - 1), total - largest - least * (amount - 1)
    while rest > 0:
        candidates = [i for i in range(1, amount) if given[i] < largest] or [i for i in range(1, amount) if given[i] < limit]
        mass, remaining = sum([loads[i] for i in candidates]), rest
        for i in candidates:
            addition = min(limit - given[i], max(1, remaining * loads[i] // mass), rest)
            given[i] = given[i] + addition
            rest = rest - addition
    return np.array(given)


def gaussian(own_key, extent, spread, most, shards=(), kind=jnp.bfloat16):
    loudness = block_scale(own_key, extent, shards, -0.22, 0.18) if shards else 1.0
    entries = jax.random.normal(own_key, extent, jnp.float32) * spread * loudness
    return jnp.minimum(jnp.maximum(entries, -most), most).astype(kind)


def setup_inputs(seed: int = 0, part: int = 0) -> dict:
    splits = jax.random.split(jax.random.key(seed), 25)
    part_keys = jax.random.split(jax.random.fold_in(splits[24], part), 25)
    tokens = gaussian(part_keys[0], (SEQS, D), 1.0, 6.0, ((0, 32),))
    routes_keys = jax.random.split(jax.random.fold_in(part_keys[1], 1), SEQS // SEQ_DEV)
    routes_turns = jax.random.permutation(jax.random.fold_in(part_keys[1], 3), SEQS // SEQ_DEV)
    routes = jax.vmap(lambda own, number: assign_block(jax.random.fold_in(part_keys[1], 2), own, number, SEQ_DEV, EXPERTS, TOPK, CAP, 2))(routes_keys, routes_turns).reshape((SEQS, TOPK))
    route_logits = gaussian(part_keys[2], (SEQS, TOPK), 1.0, 4.0, ((0, 32),), jnp.float32)
    state_real = gaussian(part_keys[3], (SEQS, GROUPS, STATE), 0.5, 4.0, ((1, 32),), jnp.float32)
    state_imag = gaussian(part_keys[4], (SEQS, GROUPS, STATE), 0.5, 4.0, ((1, 32),), jnp.float32)
    gain_in = jnp.clip(1.0 + 0.18 * jax.random.normal(splits[5], (D,), jnp.float32), 0.1, 1.9)
    proj_in = gaussian(splits[6], (D, CHANNELS), D ** -0.5, 0.125, ((1, 32),))
    decay_rate = jnp.clip(jnp.exp(math.log(2.0) - 3.6888794 * jax.random.uniform(splits[7], (GROUPS, STATE), jnp.float32) ** block_scale(splits[7], (GROUPS, STATE), ((0, 32),), -0.2, 0.2)), 0.05, 2.0)
    frequency = jnp.clip(jax.random.uniform(splits[8], (GROUPS, STATE), jnp.float32, -4.0, 4.0) * block_scale(splits[8], (GROUPS, STATE), ((0, 32),), -0.4, 0.0), -4.0, 4.0)
    log_step = jnp.clip(-3.0 + 3.0 * jax.random.uniform(splits[9], (GROUPS,), jnp.float32) ** block_scale(splits[9], (GROUPS,), ((0, 32),), -0.2, 0.2), -3.0, 0.0)
    input_real = gaussian(splits[10], (GROUPS, STATE, GROUP), (2 * GROUP) ** -0.5, 1.0, ((0, 32),), jnp.float32)
    input_imag = gaussian(splits[11], (GROUPS, STATE, GROUP), (2 * GROUP) ** -0.5, 1.0, ((0, 32),), jnp.float32)
    output_real = gaussian(splits[12], (GROUPS, GROUP, STATE), (2 * STATE) ** -0.5, 0.5, ((0, 32),), jnp.float32)
    output_imag = gaussian(splits[13], (GROUPS, GROUP, STATE), (2 * STATE) ** -0.5, 0.5, ((0, 32),), jnp.float32)
    skip_gain = gaussian(splits[14], (GROUPS, GROUP), 1.0, 4.0, ((0, 32),), jnp.float32)
    proj_out = gaussian(splits[15], (CHANNELS, D), CHANNELS ** -0.5, 0.1875, ((0, 32),))
    gain_mid = jnp.clip(1.0 + 0.18 * jax.random.normal(splits[16], (D,), jnp.float32), 0.1, 1.9)
    expert_gate = gaussian(splits[17], (EXPERTS, D, FF), (2.5 / D ** 0.5), 0.33007812, ((0, 32),))
    expert_up = gaussian(splits[18], (EXPERTS, D, FF), (2.5 / D ** 0.5), 0.33007812, ((0, 32),))
    expert_down = gaussian(splits[19], (EXPERTS, FF, D), (0.3 / FF ** 0.5), 0.056152344, ((0, 32),))
    dense_gate = gaussian(splits[20], (D, DENSE), D ** -0.5, 0.125, ((1, 32),))
    dense_up = gaussian(splits[21], (D, DENSE), D ** -0.5, 0.125, ((1, 32),))
    dense_down = gaussian(splits[22], (DENSE, D), DENSE ** -0.5, 0.125, ((0, 32),))
    dense_mix = gaussian(splits[23], (DENSE,), (3.0 / DENSE ** 0.5), 0.39774758, ((0, 32),), jnp.float32)
    return {"tokens": tokens, "routes": routes, "route_logits": route_logits, "state_real": state_real, "state_imag": state_imag, "gain_in": gain_in, "proj_in": proj_in, "decay_rate": decay_rate, "frequency": frequency, "log_step": log_step, "input_real": input_real, "input_imag": input_imag, "output_real": output_real, "output_imag": output_imag, "skip_gain": skip_gain, "proj_out": proj_out, "gain_mid": gain_mid, "expert_gate": expert_gate, "expert_up": expert_up, "expert_down": expert_down, "dense_gate": dense_gate, "dense_up": dense_up, "dense_down": dense_down, "dense_mix": dense_mix}


EPS = 1e-06
LIMIT = 7.0
ALPHA = 1.702
HIGH = lax.Precision.HIGHEST

def rms_scale(values, gain_vec):
    return values * lax.rsqrt(lax.optimization_barrier(jnp.mean(values * values, axis=-1, keepdims=True)) + EPS) * gain_vec

def state_step(unit_rows, state_real, state_imag, decay_rate, frequency, log_step, input_real, input_imag, output_real, output_imag, skip_gain):
    seq_count = unit_rows.shape[0]
    groups, group_size = skip_gain.shape
    inputs = unit_rows.astype(jnp.float32).reshape(seq_count, groups, group_size)
    step_size = jnp.exp(log_step)[:, None]
    decay_part = -decay_rate
    magnitude = jnp.exp(decay_part * step_size)
    carry_real = magnitude * jnp.cos(frequency * step_size)
    carry_imag = magnitude * jnp.sin(frequency * step_size)
    denom = decay_part * decay_part + frequency * frequency
    feed_real = ((carry_real - 1.0) * decay_part + carry_imag * frequency) / denom
    feed_imag = (carry_imag * decay_part - (carry_real - 1.0) * frequency) / denom
    drive_real = jnp.einsum('sgp,gnp->sgn', inputs, input_real, precision=HIGH)
    drive_imag = jnp.einsum('sgp,gnp->sgn', inputs, input_imag, precision=HIGH)
    new_real = carry_real * state_real - carry_imag * state_imag + feed_real * drive_real - feed_imag * drive_imag
    new_imag = carry_real * state_imag + carry_imag * state_real + feed_real * drive_imag + feed_imag * drive_real
    readout = jnp.einsum('gpn,sgn->sgp', output_real, new_real, precision=HIGH) - jnp.einsum('gpn,sgn->sgp', output_imag, new_imag, precision=HIGH) + skip_gain * inputs
    branch = jax.nn.gelu(readout).reshape(seq_count, groups * group_size).astype(jnp.bfloat16)
    return (branch, new_real, new_imag)

def expert_apply(row_block, gate_weight, up_weight, down_weight):
    gated = jnp.minimum(jnp.dot(row_block, gate_weight, preferred_element_type=jnp.float32), LIMIT)
    upper = jnp.clip(jnp.dot(row_block, up_weight, preferred_element_type=jnp.float32), -LIMIT, LIMIT)
    activated = ((upper + 1.0) * gated * jax.nn.sigmoid(ALPHA * gated)).astype(jnp.bfloat16)
    return jnp.dot(activated, down_weight, preferred_element_type=jnp.float32).astype(jnp.bfloat16)

def reference(tokens, routes, route_logits, state_real, state_imag, gain_in, proj_in, decay_rate, frequency, log_step, input_real, input_imag, output_real, output_imag, skip_gain, proj_out, gain_mid, expert_gate, expert_up, expert_down, dense_gate, dense_up, dense_down, dense_mix):
    inputs = tokens.astype(jnp.float32)
    normed = rms_scale(inputs, gain_in).astype(jnp.bfloat16)
    unit_rows = jnp.dot(normed, proj_in, preferred_element_type=jnp.float32).astype(jnp.bfloat16)
    branch, new_real, new_imag = state_step(unit_rows, state_real, state_imag, decay_rate, frequency, log_step, input_real, input_imag, output_real, output_imag, skip_gain)
    residual = inputs + jnp.dot(branch, proj_out, preferred_element_type=jnp.float32)
    mixed = rms_scale(residual, gain_mid).astype(jnp.bfloat16)
    weights = jnp.exp(route_logits)
    weights = weights / lax.optimization_barrier(jnp.sum(weights, axis=1, keepdims=True))
    limit_rows = N_EP * CAP
    expert_count = expert_gate.shape[0]

    def one_expert(running, expert_index):
        shares = lax.optimization_barrier(jnp.sum(jnp.where(routes == expert_index, weights, 0.0), axis=1))
        marked = jnp.any(routes == expert_index, axis=1).astype(jnp.int32)
        order_rows = jnp.argsort(1 - marked, stable=True)[:limit_rows].astype(jnp.int32)
        picked = jnp.take(mixed, order_rows, axis=0)
        result = expert_apply(picked, expert_gate[expert_index], expert_up[expert_index], expert_down[expert_index])
        running = running.at[order_rows].add(shares[order_rows][:, None] * result.astype(jnp.float32))
        return (running, None)
    routed, _ = lax.scan(one_expert, jnp.zeros(residual.shape, jnp.float32), jnp.arange(expert_count, dtype=jnp.int32))
    hidden = (jax.nn.silu(jnp.dot(mixed, dense_gate, preferred_element_type=jnp.float32)) * jnp.dot(mixed, dense_up, preferred_element_type=jnp.float32)).astype(jnp.bfloat16)
    dense_out = jnp.dot(hidden, dense_down, preferred_element_type=jnp.float32)
    gate_logit = jnp.dot(hidden.astype(jnp.float32), dense_mix, precision=HIGH)
    layer_out = (residual + routed + jax.nn.sigmoid(gate_logit)[:, None] * dense_out).astype(jnp.bfloat16)
    return (layer_out, new_real, new_imag)
```

```python
import jax
import jax.numpy as jnp
from jax import lax
from jax.sharding import Mesh
from jax.sharding import PartitionSpec as P

EP = ("chip", "core")
GRP_EP = ("grp", "chip", "core")

EPS = 1e-06
LIMIT = 7.0
ALPHA = 1.702

TOKEN_SCALE = 2.0**12
BRANCH_SCALE = 2.0**-4
PROJ_SCALE = TOKEN_SCALE / BRANCH_SCALE
SHARE_SCALE = 2.0**12

F32 = jnp.float32
BF16 = jnp.bfloat16
F16 = jnp.float16


def state_step(
    inputs,
    state_real,
    state_imag,
    decay_rate,
    frequency,
    log_step,
    input_real,
    input_imag,
    output_real,
    output_imag,
    skip_gain,
):
    seq_count = inputs.shape[0]
    groups, group_size = skip_gain.shape
    inputs = inputs.astype(F32).reshape(seq_count, groups, group_size)
    step_size = jnp.exp(log_step)[:, None]
    decay_part = -decay_rate
    magnitude = jnp.exp(decay_part * step_size)
    carry_real = magnitude * jnp.cos(frequency * step_size)
    carry_imag = magnitude * jnp.sin(frequency * step_size)
    denom = decay_part * decay_part + frequency * frequency
    feed_real = ((carry_real - 1.0) * decay_part + carry_imag * frequency) / denom
    feed_imag = (carry_imag * decay_part - (carry_real - 1.0) * frequency) / denom
    drive_real = jnp.einsum("sgp,gnp->sgn", inputs, input_real)
    drive_imag = jnp.einsum("sgp,gnp->sgn", inputs, input_imag)
    new_real = (
        carry_real * state_real
        - carry_imag * state_imag
        + feed_real * drive_real
        - feed_imag * drive_imag
    )
    new_imag = (
        carry_real * state_imag
        + carry_imag * state_real
        + feed_real * drive_imag
        + feed_imag * drive_real
    )
    readout = (
        jnp.einsum("gpn,sgn->sgp", output_real, new_real)
        - jnp.einsum("gpn,sgn->sgp", output_imag, new_imag)
        + skip_gain * inputs
    )
    branch = jax.nn.gelu(readout).reshape(seq_count, groups * group_size)
    return (branch, new_real, new_imag)


def swap(x):
    return lax.ppermute(x, "core", [(0, 1), (1, 0)])


def reduce_ring(blocks):
    chips = blocks.shape[0]
    chip = lax.axis_index("chip")
    up = [(i, (i + 1) % chips) for i in range(chips)]
    down = [(i, (i - 1) % chips) for i in range(chips)]

    def part(k):
        return lax.dynamic_index_in_dim(blocks, (chip + k) % chips, 0, keepdims=False).astype(F32)

    far_up = chips // 2
    far_down = chips - 1 - far_up
    going_up = part(far_up).astype(BF16)
    going_down = part(-far_down).astype(BF16)
    for s in range(1, far_up + 1):
        going_up = lax.ppermute(going_up, "chip", up)
        if s < far_up:
            going_up = (going_up.astype(F32) + part(far_up - s)).astype(BF16)
        if s <= far_down:
            going_down = lax.ppermute(going_down, "chip", down)
            if s < far_down:
                going_down = (going_down.astype(F32) + part(s - far_down)).astype(BF16)
    return part(0) + going_up.astype(F32) + going_down.astype(F32)


def on_device(
    tokens,
    routes,
    route_logits,
    state_real,
    state_imag,
    gain_in,
    proj_in,
    decay_rate,
    frequency,
    log_step,
    input_real,
    input_imag,
    output_real,
    output_imag,
    skip_gain,
    proj_out,
    gain_mid,
    expert_gate,
    expert_up,
    expert_down,
    dense_gate,
    dense_up,
    dense_down,
    dense_mix,
):
    chips = lax.axis_size("chip")
    cores = lax.axis_size("core")
    devices = chips * cores
    chip = lax.axis_index("chip")
    core = lax.axis_index("core")
    rows, width = tokens.shape
    top_count = routes.shape[1]
    capacity = max(2, 2 * rows * top_count // devices)
    half = chips * rows
    slots = chips * capacity

    shares = jnp.exp(route_logits)
    shares = shares / jnp.sum(shares, axis=1, keepdims=True) * SHARE_SCALE
    shares_high = shares.astype(F16)
    shares_low = (shares - shares_high.astype(F32)).astype(F16)
    routing = jnp.concatenate([routes.astype(F16), shares_high, shares_low], axis=1)
    sent = jnp.stack(
        [
            (tokens.astype(F32) * TOKEN_SCALE).astype(F16),
            (proj_out.astype(F32) * PROJ_SCALE).astype(F16),
        ]
    )
    gathered = lax.all_gather(sent, EP, axis=0, tiled=False)
    all_proj = gathered[:, 1].reshape(-1, width)
    gate_pair = jnp.concatenate([dense_gate, swap(dense_gate)], axis=1)
    up_pair = jnp.concatenate([dense_up, swap(dense_up)], axis=1)
    down_pair = jnp.concatenate([dense_down, swap(dense_down)], axis=0)
    mix_pair = jnp.concatenate([dense_mix, swap(dense_mix)], axis=0)

    wide = gathered[:, 0].reshape(-1, width).astype(F32)
    mean_in = jnp.mean(wide * wide, axis=-1, keepdims=True) * (1.0 / TOKEN_SCALE**2)
    row_scale = lax.rsqrt(mean_in + EPS) * (1.0 / TOKEN_SCALE)
    gained = (gain_in[:, None] * proj_in.astype(F32)).astype(BF16)
    units = jnp.dot(wide.astype(BF16), gained, preferred_element_type=F32) * row_scale
    branch, new_real, new_imag = state_step(
        units.astype(BF16),
        state_real,
        state_imag,
        decay_rate,
        frequency,
        log_step,
        input_real,
        input_imag,
        output_real,
        output_imag,
        skip_gain,
    )
    by_core = (branch * BRANCH_SCALE).astype(F16).T.reshape(-1, chips, cores, rows)

    def half_of(index):
        return lax.dynamic_index_in_dim(by_core, index, 2, keepdims=False).reshape(-1, half)

    kept, got = half_of(core), swap(half_of(1 - core))
    both = jnp.where(
        core == 0, jnp.concatenate([kept, got], axis=0), jnp.concatenate([got, kept], axis=0)
    )
    routing_row = jnp.pad(routing.T.reshape(1, -1), ((0, 7), (0, half - routing.size)))
    branch_and_routing = lax.all_gather(
        jnp.concatenate([both, routing_row], axis=0), "chip", axis=0, tiled=False
    )
    channels = both.shape[0]
    all_branch = branch_and_routing[:, :channels].reshape(-1, half).astype(BF16)
    all_routing = branch_and_routing[:, channels, : routing.size].reshape(chips, 3, top_count, rows)
    mixer_out = lax.dot_general(
        all_branch,
        all_proj.astype(BF16),
        (((0,), (0,)), ((), ())),
        preferred_element_type=F32,
    )
    tokens_half = lax.dynamic_index_in_dim(
        gathered[:, 0].reshape(chips, cores, rows, width), core, 1, keepdims=False
    ).reshape(half, width)
    residual = (tokens_half.astype(F32) + mixer_out) * (1.0 / TOKEN_SCALE)
    mean_mid = jnp.mean(residual * residual, axis=-1, keepdims=True)
    mixed = (residual * lax.rsqrt(mean_mid + EPS) * gain_mid).astype(BF16)

    hidden = (
        jax.nn.silu(jnp.dot(mixed, gate_pair, preferred_element_type=F32))
        * jnp.dot(mixed, up_pair, preferred_element_type=F32)
    ).astype(BF16)
    logit_term = jnp.sum(hidden.astype(F32) * mix_pair, axis=1)
    logit_terms = lax.all_to_all(
        jnp.broadcast_to(logit_term[None], (chips, half)), "chip", 0, 0, tiled=True
    )

    table = all_routing.astype(F32)
    names = table[:, 0]
    weights = (table[:, 1] + table[:, 2]) * (1.0 / SHARE_SCALE)
    before = (jnp.arange(rows)[:, None] < jnp.arange(rows)[None, :]).astype(BF16)

    def places(expert, base):
        hit = names == expert.astype(F32)
        share = jnp.sum(jnp.where(hit, weights, 0.0), axis=1)
        marked = jnp.any(hit, axis=1)
        rank = jnp.dot(marked.astype(BF16), before, preferred_element_type=F32)
        first = (base + jnp.arange(chips) * capacity)[:, None].astype(F32)
        return (jnp.where(marked, first + rank, -1.0).reshape(half), share.reshape(half))

    own_place, own_share = places(chip * cores + core, 0)
    pair_place, pair_share = places(chip * cores + (1 - core), slots)
    slot_ids = jnp.arange(cores * slots).astype(F32)
    of_own = own_place[None, :] == slot_ids[:, None]
    of_pair = pair_place[None, :] == slot_ids[:, None]
    slot_share = jnp.sum(
        jnp.where(of_own, own_share[None, :], 0.0) + jnp.where(of_pair, pair_share[None, :], 0.0),
        axis=1,
        keepdims=True,
    )
    selector = (of_own | of_pair).astype(BF16)
    picked = jnp.dot(selector, mixed, preferred_element_type=F32).astype(BF16)
    picked = jnp.concatenate([picked[:slots], swap(picked[slots:])], axis=0)
    gated = jnp.minimum(jnp.dot(picked, expert_gate[0], preferred_element_type=F32), LIMIT)
    upper = jnp.clip(jnp.dot(picked, expert_up[0], preferred_element_type=F32), -LIMIT, LIMIT)
    activated = ((upper + 1.0) * gated * jax.nn.sigmoid(ALPHA * gated)).astype(BF16)
    result = jnp.dot(activated, expert_down[0], preferred_element_type=F32).astype(BF16)
    result = jnp.concatenate([result[:slots], swap(result[slots:])], axis=0)
    result = (result.astype(F32) * slot_share).astype(BF16)

    placing = (
        (own_place[:, None] == slot_ids[None, :]) | (pair_place[:, None] == slot_ids[None, :])
    ).astype(BF16)
    gate_weight = jax.nn.sigmoid(jnp.sum(logit_terms, axis=0))
    gated_hidden = (gate_weight[:, None] * hidden.astype(F32)).astype(BF16)
    combined = jnp.dot(
        jnp.concatenate([gated_hidden, placing], axis=1),
        jnp.concatenate([down_pair, result], axis=0),
        preferred_element_type=F32,
    ).astype(BF16)
    summed = reduce_ring(combined.reshape(chips, rows, width))
    own_residual = lax.dynamic_slice_in_dim(residual, chip * rows, rows, 0)
    layer_out = (own_residual + summed).astype(BF16)
    return (layer_out, new_real, new_imag)


def solution(mesh):
    cores = 2
    split = Mesh(
        mesh.devices.reshape(mesh.shape["grp"], mesh.shape["ep"] // cores, cores),
        ("grp", "chip", "core"),
    )
    return jax.shard_map(
        on_device,
        mesh=split,
        in_specs=(
            P(GRP_EP, None),
            P(GRP_EP, None),
            P(GRP_EP, None),
            P("grp", EP, None),
            P("grp", EP, None),
            P(),
            P(None, EP),
            P(EP, None),
            P(EP, None),
            P(EP),
            P(EP, None, None),
            P(EP, None, None),
            P(EP, None, None),
            P(EP, None, None),
            P(EP, None),
            P(EP, None),
            P(),
            P(EP, None, None),
            P(EP, None, None),
            P(EP, None, None),
            P(None, EP),
            P(None, EP),
            P(EP, None),
            P(EP),
        ),
        out_specs=(P(GRP_EP, None), P("grp", EP, None), P("grp", EP, None)),
        check_vma=False,
    )
```

```python
import jax
import jax.numpy as jnp
from jax import lax
from jax.experimental import pallas as pl
from jax.experimental.pallas import tpu as pltpu
from jax.sharding import Mesh
from jax.sharding import PartitionSpec as P

EP = ("chip", "core")
GRP_EP = ("grp", "chip", "core")

EPS = 1e-06
LIMIT = 7.0
ALPHA = 1.702

TOKEN_SCALE = 2.0**12
BRANCH_SCALE = 2.0**-4
PROJ_SCALE = TOKEN_SCALE / BRANCH_SCALE
SHARE_SCALE = 2.0**12

MIXER_STEPS = 2
EXPERT_STEPS = 2

F32 = jnp.float32
BF16 = jnp.bfloat16
F16 = jnp.float16


def state_step(
    inputs,
    state_real,
    state_imag,
    decay_rate,
    frequency,
    log_step,
    input_real,
    input_imag,
    output_real,
    output_imag,
    skip_gain,
):
    seq_count = inputs.shape[0]
    groups, group_size = skip_gain.shape
    inputs = inputs.astype(F32).reshape(seq_count, groups, group_size)
    step_size = jnp.exp(log_step)[:, None]
    decay_part = -decay_rate
    magnitude = jnp.exp(decay_part * step_size)
    carry_real = magnitude * jnp.cos(frequency * step_size)
    carry_imag = magnitude * jnp.sin(frequency * step_size)
    denom = decay_part * decay_part + frequency * frequency
    feed_real = ((carry_real - 1.0) * decay_part + carry_imag * frequency) / denom
    feed_imag = (carry_imag * decay_part - (carry_real - 1.0) * frequency) / denom
    drive_real = jnp.einsum("sgp,gnp->sgn", inputs, input_real)
    drive_imag = jnp.einsum("sgp,gnp->sgn", inputs, input_imag)
    new_real = (
        carry_real * state_real
        - carry_imag * state_imag
        + feed_real * drive_real
        - feed_imag * drive_imag
    )
    new_imag = (
        carry_real * state_imag
        + carry_imag * state_real
        + feed_real * drive_imag
        + feed_imag * drive_real
    )
    readout = (
        jnp.einsum("gpn,sgn->sgp", output_real, new_real)
        - jnp.einsum("gpn,sgn->sgp", output_imag, new_imag)
        + skip_gain * inputs
    )
    branch = jax.nn.gelu(readout).reshape(seq_count, groups * group_size)
    return (branch, new_real, new_imag)


def swap(x):
    return lax.ppermute(x, "core", [(0, 1), (1, 0)])


def reduce_ring(blocks):
    chips = blocks.shape[0]
    chip = lax.axis_index("chip")
    up = [(i, (i + 1) % chips) for i in range(chips)]
    down = [(i, (i - 1) % chips) for i in range(chips)]

    def part(k):
        return lax.dynamic_index_in_dim(blocks, (chip + k) % chips, 0, keepdims=False).astype(F32)

    far_up = chips // 2
    far_down = chips - 1 - far_up
    going_up = part(far_up).astype(BF16)
    going_down = part(-far_down).astype(BF16)
    for s in range(1, far_up + 1):
        going_up = lax.ppermute(going_up, "chip", up)
        if s < far_up:
            going_up = (going_up.astype(F32) + part(far_up - s)).astype(BF16)
        if s <= far_down:
            going_down = lax.ppermute(going_down, "chip", down)
            if s < far_down:
                going_down = (going_down.astype(F32) + part(s - far_down)).astype(BF16)
    return part(0) + going_up.astype(F32) + going_down.astype(F32)


def mixer_kernel(place, branch, proj, tokens, gain, mixed, own, total):
    rows, block = own.shape[0], total.shape[0]
    total[...] = (
        tokens[...].reshape(total.shape).astype(F32)
        + lax.dot_general(
            branch[...], proj[...], (((0,), (0,)), ((), ())), preferred_element_type=F32
        )
    ) * (1.0 / TOKEN_SCALE)
    values = total[...]
    mean = jnp.mean(values * values, axis=-1, keepdims=True)
    mixed[...] = (values * lax.rsqrt(mean + EPS) * gain[...]).astype(BF16)
    at = place[0] * rows

    @pl.when(at // block == pl.program_id(0))
    def _():
        own[...] = total[pl.ds(pl.multiple_of(at % block, rows), rows), :]


def mixer(place, branch, proj, tokens, gain):
    chips, _, rows, width = tokens.shape
    held = chips // MIXER_STEPS
    whole = lambda i, place: (0, 0)
    return pl.pallas_call(
        mixer_kernel,
        grid_spec=pltpu.PrefetchScalarGridSpec(
            num_scalar_prefetch=1,
            grid=(MIXER_STEPS,),
            in_specs=[
                pl.BlockSpec((branch.shape[0], held * rows), lambda i, place: (0, i)),
                pl.BlockSpec(proj.shape, whole),
                pl.BlockSpec((held, 1, rows, width), lambda i, place: (i, place[1], 0, 0)),
                pl.BlockSpec((1, width), whole),
            ],
            out_specs=[
                pl.BlockSpec((held * rows, width), lambda i, place: (i, 0)),
                pl.BlockSpec((rows, width), whole),
            ],
            scratch_shapes=[pltpu.VMEM((held * rows, width), F32)],
        ),
        out_shape=[
            jax.ShapeDtypeStruct((chips * rows, width), BF16),
            jax.ShapeDtypeStruct((rows, width), F32),
        ],
        compiler_params=pltpu.CompilerParams(vmem_limit_bytes=48 * 2**20),
        name="mixer",
    )(place, branch, proj, tokens, gain.reshape(1, width))


def expert_kernel(picked, gate, up, down, result, total):
    gated = jnp.minimum(jnp.dot(picked[...], gate[0], preferred_element_type=F32), LIMIT)
    upper = jnp.clip(jnp.dot(picked[...], up[0], preferred_element_type=F32), -LIMIT, LIMIT)
    activated = ((upper + 1.0) * gated * jax.nn.sigmoid(ALPHA * gated)).astype(BF16)
    part = jnp.dot(activated, down[0], preferred_element_type=F32)

    @pl.when(pl.program_id(0) == 0)
    def _():
        total[...] = part

    @pl.when(pl.program_id(0) > 0)
    def _():
        total[...] += part

    @pl.when(pl.program_id(0) == pl.num_programs(0) - 1)
    def _():
        result[...] = total[...].astype(BF16)


def expert_apply(picked, gate, up, down):
    count, width = picked.shape
    hidden = gate.shape[2]
    block = hidden // EXPERT_STEPS
    return pl.pallas_call(
        expert_kernel,
        grid=(hidden // block,),
        in_specs=[
            pl.BlockSpec((count, width), lambda i: (0, 0)),
            pl.BlockSpec((1, width, block), lambda i: (0, 0, i)),
            pl.BlockSpec((1, width, block), lambda i: (0, 0, i)),
            pl.BlockSpec((1, block, width), lambda i: (0, i, 0)),
        ],
        out_specs=pl.BlockSpec((count, width), lambda i: (0, 0)),
        out_shape=jax.ShapeDtypeStruct((count, width), BF16),
        scratch_shapes=[pltpu.VMEM((count, width), F32)],
        compiler_params=pltpu.CompilerParams(vmem_limit_bytes=48 * 2**20),
        name="expert",
    )(picked, gate, up, down)


def on_device(
    tokens,
    routes,
    route_logits,
    state_real,
    state_imag,
    gain_in,
    proj_in,
    decay_rate,
    frequency,
    log_step,
    input_real,
    input_imag,
    output_real,
    output_imag,
    skip_gain,
    proj_out,
    gain_mid,
    expert_gate,
    expert_up,
    expert_down,
    dense_gate,
    dense_up,
    dense_down,
    dense_mix,
):
    chips = lax.axis_size("chip")
    cores = lax.axis_size("core")
    devices = chips * cores
    chip = lax.axis_index("chip")
    core = lax.axis_index("core")
    rows, width = tokens.shape
    top_count = routes.shape[1]
    capacity = max(2, 2 * rows * top_count // devices)
    half = chips * rows
    slots = chips * capacity

    shares = jnp.exp(route_logits)
    shares = shares / jnp.sum(shares, axis=1, keepdims=True) * SHARE_SCALE
    shares_high = shares.astype(F16)
    shares_low = (shares - shares_high.astype(F32)).astype(F16)
    routing = jnp.concatenate([routes.astype(F16), shares_high, shares_low], axis=1)
    sent = jnp.stack(
        [
            (tokens.astype(F32) * TOKEN_SCALE).astype(F16),
            (proj_out.astype(F32) * PROJ_SCALE).astype(F16),
        ]
    )
    gathered = lax.all_gather(sent, EP, axis=0, tiled=False)
    all_tokens, all_proj = lax.optimization_barrier(
        (
            gathered[:, 0].reshape(-1, width).astype(BF16),
            gathered[:, 1].reshape(-1, width).astype(BF16),
        )
    )
    own_dense = jnp.concatenate([dense_gate.T, dense_up.T], axis=0)
    dense_pair = jnp.concatenate([own_dense, swap(own_dense)], axis=0)
    down_pair = jnp.concatenate([dense_down, swap(dense_down)], axis=0)
    mix_pair = jnp.concatenate([dense_mix, swap(dense_mix)], axis=0)

    wide = all_tokens.astype(F32)
    mean_in = jnp.mean(wide * wide, axis=-1, keepdims=True) * (1.0 / TOKEN_SCALE**2)
    row_scale = lax.rsqrt(mean_in + EPS) * (1.0 / TOKEN_SCALE)
    gained = (gain_in[:, None] * proj_in.astype(F32)).astype(BF16)
    units = jnp.dot(all_tokens, gained, preferred_element_type=F32) * row_scale
    branch, new_real, new_imag = state_step(
        units.astype(BF16),
        state_real,
        state_imag,
        decay_rate,
        frequency,
        log_step,
        input_real,
        input_imag,
        output_real,
        output_imag,
        skip_gain,
    )
    by_core = (branch * BRANCH_SCALE).astype(F16).T.reshape(-1, chips, cores, rows)

    def half_of(index):
        return lax.dynamic_index_in_dim(by_core, index, 2, keepdims=False).reshape(-1, half)

    kept, got = half_of(core), swap(half_of(1 - core))
    both = jnp.where(
        core == 0, jnp.concatenate([kept, got], axis=0), jnp.concatenate([got, kept], axis=0)
    )
    lanes = jnp.arange(half)
    routing_rows = jnp.where(lanes // rows == chip, jnp.tile(routing.T, (1, chips)), 0.0)
    routing_rows = jnp.pad(routing_rows.astype(F16), ((0, 16 - 3 * top_count), (0, 0)))
    branch_and_routing = lax.all_gather(
        jnp.concatenate([both, routing_rows], axis=0), "chip", axis=0, tiled=False
    )
    channels = both.shape[0]
    all_branch = branch_and_routing[:, :channels].reshape(-1, half).astype(BF16)
    mixed, own_residual = mixer(
        jnp.stack([chip, core]),
        all_branch,
        all_proj,
        all_tokens.reshape(chips, cores, rows, width),
        gain_mid,
    )

    products = lax.dot_general(
        dense_pair, mixed, (((1,), (1,)), ((), ())), preferred_element_type=F32
    ).reshape(cores, 2, -1, half)
    hidden = (jax.nn.silu(products[:, 0]) * products[:, 1]).astype(BF16).reshape(-1, half)
    logit_term = jnp.sum(hidden.astype(F32) * mix_pair[:, None], axis=0)
    logit_terms = lax.all_to_all(
        jnp.broadcast_to(logit_term[None], (chips, half)), "chip", 0, 0, tiled=True
    )

    table = jnp.sum(branch_and_routing[:, channels : channels + 3 * top_count].astype(F32), axis=0)
    names = table[:top_count]
    weights = (table[top_count : 2 * top_count] + table[2 * top_count :]) * (1.0 / SHARE_SCALE)
    before = (
        (lanes[:, None] < lanes[None, :]) & (lanes[:, None] // rows == lanes[None, :] // rows)
    ).astype(BF16)
    first = (lanes // rows * capacity).astype(F32)[None, :]
    slot_ids = jnp.arange(slots).astype(F32)[:, None]

    def slot_table(expert):
        hit = names == expert.astype(F32)
        share = jnp.sum(jnp.where(hit, weights, 0.0), axis=0, keepdims=True)
        marked = jnp.any(hit, axis=0, keepdims=True)
        rank = jnp.dot(marked.astype(BF16), before, preferred_element_type=F32)
        chosen = jnp.where(marked, first + rank, -1.0) == slot_ids
        return (chosen, jnp.sum(jnp.where(chosen, share, 0.0), axis=1, keepdims=True))

    own_chosen, own_share = slot_table(chip * cores + core)
    pair_chosen, pair_share = slot_table(chip * cores + (1 - core))
    selector = jnp.concatenate([own_chosen, pair_chosen], axis=0).astype(BF16)
    slot_share = jnp.concatenate([own_share, pair_share], axis=0)
    picked = jnp.dot(selector, mixed, preferred_element_type=F32).astype(BF16)
    picked = jnp.concatenate([picked[:slots], swap(picked[slots:])], axis=0)
    result = expert_apply(picked, expert_gate, expert_up, expert_down)
    result = jnp.concatenate([result[:slots], swap(result[slots:])], axis=0)
    result = (result.astype(F32) * slot_share).astype(BF16)

    gate_weight = jax.nn.sigmoid(jnp.sum(logit_terms, axis=0, keepdims=True))
    gated_hidden = (gate_weight * hidden.astype(F32)).astype(BF16)
    combined = lax.dot_general(
        jnp.concatenate([gated_hidden, selector], axis=0),
        jnp.concatenate([down_pair, result], axis=0),
        (((0,), (0,)), ((), ())),
        preferred_element_type=F32,
    ).astype(BF16)
    summed = reduce_ring(combined.reshape(chips, rows, width))
    layer_out = (own_residual + summed).astype(BF16)
    return (layer_out, new_real, new_imag)


def solution(mesh):
    cores = 2
    split = Mesh(
        mesh.devices.reshape(mesh.shape["grp"], mesh.shape["ep"] // cores, cores),
        ("grp", "chip", "core"),
    )
    return jax.shard_map(
        on_device,
        mesh=split,
        in_specs=(
            P(GRP_EP, None),
            P(GRP_EP, None),
            P(GRP_EP, None),
            P("grp", EP, None),
            P("grp", EP, None),
            P(),
            P(None, EP),
            P(EP, None),
            P(EP, None),
            P(EP),
            P(EP, None, None),
            P(EP, None, None),
            P(EP, None, None),
            P(EP, None, None),
            P(EP, None),
            P(EP, None),
            P(),
            P(EP, None, None),
            P(EP, None, None),
            P(EP, None, None),
            P(None, EP),
            P(None, EP),
            P(EP, None),
            P(EP),
        ),
        out_specs=(P(GRP_EP, None), P("grp", EP, None), P("grp", EP, None)),
        check_vma=False,
    )
```

```python
import jax
import jax.numpy as jnp
from jax import lax
from jax.experimental import pallas as pl
from jax.experimental.pallas import tpu as pltpu
from jax.sharding import Mesh
from jax.sharding import PartitionSpec as P

EP = ("chip", "core")
GRP_EP = ("grp", "chip", "core")

EPS = 1e-06
LIMIT = 7.0
ALPHA = 1.702

TOKEN_SCALE = 2.0**12
BRANCH_SCALE = 2.0**-4
PROJ_SCALE = TOKEN_SCALE / BRANCH_SCALE
SHARE_SCALE = 2.0**12

MIXER_STEPS = 2
EXPERT_STEPS = 2
REDUCE_PARTS = 2

F32 = jnp.float32
BF16 = jnp.bfloat16
F16 = jnp.float16


def state_step(
    inputs,
    state_real,
    state_imag,
    decay_rate,
    frequency,
    log_step,
    input_real,
    input_imag,
    output_real,
    output_imag,
    skip_gain,
):
    seq_count = inputs.shape[0]
    groups, group_size = skip_gain.shape
    inputs = inputs.astype(F32).reshape(seq_count, groups, group_size)
    step_size = jnp.exp(log_step)[:, None]
    decay_part = -decay_rate
    magnitude = jnp.exp(decay_part * step_size)
    carry_real = magnitude * jnp.cos(frequency * step_size)
    carry_imag = magnitude * jnp.sin(frequency * step_size)
    denom = decay_part * decay_part + frequency * frequency
    feed_real = ((carry_real - 1.0) * decay_part + carry_imag * frequency) / denom
    feed_imag = (carry_imag * decay_part - (carry_real - 1.0) * frequency) / denom
    drive_real = jnp.einsum("sgp,gnp->sgn", inputs, input_real)
    drive_imag = jnp.einsum("sgp,gnp->sgn", inputs, input_imag)
    new_real = (
        carry_real * state_real
        - carry_imag * state_imag
        + feed_real * drive_real
        - feed_imag * drive_imag
    )
    new_imag = (
        carry_real * state_imag
        + carry_imag * state_real
        + feed_real * drive_imag
        + feed_imag * drive_real
    )
    readout = (
        jnp.einsum("gpn,sgn->sgp", output_real, new_real)
        - jnp.einsum("gpn,sgn->sgp", output_imag, new_imag)
        + skip_gain * inputs
    )
    branch = jax.nn.gelu(readout).reshape(seq_count, groups * group_size)
    return (branch, new_real, new_imag)


def swap(x):
    return lax.ppermute(x, "core", [(0, 1), (1, 0)])


def reduce_to_own(blocks):
    chips = blocks.shape[0]
    cores = lax.axis_size("core")
    chip = lax.axis_index("chip")
    core = lax.axis_index("core")
    span = (chips - 1) // 3
    reach = span // 2
    assert chips == 3 * (2 * reach + 1) + 1

    def part(k):
        return lax.dynamic_index_in_dim(blocks, (chip + k) % chips, 0, keepdims=False).astype(F32)

    def send(x, hops):
        pairs = [(i, (i + hops) % chips) for i in range(chips)]
        return lax.ppermute(x.astype(BF16), "chip", pairs).astype(F32)

    def send_both_ways(x, hops):
        pairs = [
            (i * cores + c, (i + (hops if c == 0 else -hops)) % chips * cores + c)
            for i in range(chips)
            for c in range(cores)
        ]
        return lax.ppermute(x.astype(BF16), ("chip", "core"), pairs).astype(F32)

    far = chips // 2
    up = jnp.stack([part(span + reach), part(reach - span), part(reach)])
    down = jnp.stack([part(-span - reach), part(span - reach), part(-reach)])
    left_over = send_both_ways(part(far), far - (span + reach - 1))
    for s in range(reach - 1, -1, -1):
        up, down = send(up, 1), send(down, -1)
        if s > 0:
            up = up + jnp.stack([part(span + s), part(s - span), part(s)])
            down = down + jnp.stack([part(-span - s), part(span - s), part(-s)])
        if s == reach - 1:
            up = up.at[0].add(jnp.where(core == 0, left_over, 0.0))
            down = down.at[0].add(jnp.where(core == 0, 0.0, left_over))
    from_below = send(part(span) + up[0] + down[1], span)
    from_above = send(part(-span) + up[1] + down[0], -span)
    return part(0) + up[2] + down[2] + from_below + from_above


def mixer_kernel(place, branch, proj, tokens, gain, mixed, own, total):
    rows, block = own.shape[0], total.shape[0]
    total[...] = (
        tokens[...].reshape(total.shape).astype(F32)
        + lax.dot_general(
            branch[...], proj[...], (((0,), (0,)), ((), ())), preferred_element_type=F32
        )
    ) * (1.0 / TOKEN_SCALE)
    values = total[...]
    mean = jnp.mean(values * values, axis=-1, keepdims=True)
    mixed[...] = (values * lax.rsqrt(mean + EPS) * gain[...]).astype(BF16)
    at = place[0] * rows

    @pl.when(at // block == pl.program_id(0))
    def _():
        own[...] = total[pl.ds(pl.multiple_of(at % block, rows), rows), :]


def mixer(place, branch, proj, tokens, gain):
    chips, _, rows, width = tokens.shape
    held = chips // MIXER_STEPS
    whole = lambda i, place: (0, 0)
    return pl.pallas_call(
        mixer_kernel,
        grid_spec=pltpu.PrefetchScalarGridSpec(
            num_scalar_prefetch=1,
            grid=(MIXER_STEPS,),
            in_specs=[
                pl.BlockSpec((branch.shape[0], held * rows), lambda i, place: (0, i)),
                pl.BlockSpec(proj.shape, whole),
                pl.BlockSpec((held, 1, rows, width), lambda i, place: (i, place[1], 0, 0)),
                pl.BlockSpec((1, width), whole),
            ],
            out_specs=[
                pl.BlockSpec((held * rows, width), lambda i, place: (i, 0)),
                pl.BlockSpec((rows, width), whole),
            ],
            scratch_shapes=[pltpu.VMEM((held * rows, width), F32)],
        ),
        out_shape=[
            jax.ShapeDtypeStruct((chips * rows, width), BF16),
            jax.ShapeDtypeStruct((rows, width), F32),
        ],
        compiler_params=pltpu.CompilerParams(vmem_limit_bytes=48 * 2**20),
        name="mixer",
    )(place, branch, proj, tokens, gain.reshape(1, width))


def expert_kernel(picked, gate, up, down, result, total):
    gated = jnp.minimum(jnp.dot(picked[...], gate[0], preferred_element_type=F32), LIMIT)
    upper = jnp.clip(jnp.dot(picked[...], up[0], preferred_element_type=F32), -LIMIT, LIMIT)
    activated = ((upper + 1.0) * gated * jax.nn.sigmoid(ALPHA * gated)).astype(BF16)
    part = jnp.dot(activated, down[0], preferred_element_type=F32)

    @pl.when(pl.program_id(0) == 0)
    def _():
        total[...] = part

    @pl.when(pl.program_id(0) > 0)
    def _():
        total[...] += part

    @pl.when(pl.program_id(0) == pl.num_programs(0) - 1)
    def _():
        result[...] = total[...].astype(BF16)


def expert_apply(picked, gate, up, down):
    count, width = picked.shape
    hidden = gate.shape[2]
    block = hidden // EXPERT_STEPS
    return pl.pallas_call(
        expert_kernel,
        grid=(hidden // block,),
        in_specs=[
            pl.BlockSpec((count, width), lambda i: (0, 0)),
            pl.BlockSpec((1, width, block), lambda i: (0, 0, i)),
            pl.BlockSpec((1, width, block), lambda i: (0, 0, i)),
            pl.BlockSpec((1, block, width), lambda i: (0, i, 0)),
        ],
        out_specs=pl.BlockSpec((count, width), lambda i: (0, 0)),
        out_shape=jax.ShapeDtypeStruct((count, width), BF16),
        scratch_shapes=[pltpu.VMEM((count, width), F32)],
        compiler_params=pltpu.CompilerParams(vmem_limit_bytes=48 * 2**20),
        name="expert",
    )(picked, gate, up, down)


def on_device(
    tokens,
    routes,
    route_logits,
    state_real,
    state_imag,
    gain_in,
    proj_in,
    decay_rate,
    frequency,
    log_step,
    input_real,
    input_imag,
    output_real,
    output_imag,
    skip_gain,
    proj_out,
    gain_mid,
    expert_gate,
    expert_up,
    expert_down,
    dense_gate,
    dense_up,
    dense_down,
    dense_mix,
):
    chips = lax.axis_size("chip")
    cores = lax.axis_size("core")
    devices = chips * cores
    chip = lax.axis_index("chip")
    core = lax.axis_index("core")
    rows, width = tokens.shape
    top_count = routes.shape[1]
    capacity = max(2, 2 * rows * top_count // devices)
    half = chips * rows
    slots = chips * capacity

    shares = jnp.exp(route_logits)
    shares = shares / jnp.sum(shares, axis=1, keepdims=True) * SHARE_SCALE
    shares_high = shares.astype(F16)
    shares_low = (shares - shares_high.astype(F32)).astype(F16)
    routing = jnp.concatenate([routes.astype(F16), shares_high, shares_low], axis=1)
    sent = jnp.stack(
        [
            (tokens.astype(F32) * TOKEN_SCALE).astype(F16),
            (proj_out.astype(F32) * PROJ_SCALE).astype(F16),
        ]
    )
    gathered = lax.all_gather(sent, EP, axis=0, tiled=False)
    all_tokens, all_proj = lax.optimization_barrier(
        (
            gathered[:, 0].reshape(-1, width).astype(BF16),
            gathered[:, 1].reshape(-1, width).astype(BF16),
        )
    )
    own_dense = jnp.concatenate([dense_gate.T, dense_up.T], axis=0)
    dense_pair = jnp.concatenate([own_dense, swap(own_dense)], axis=0)
    down_pair = jnp.concatenate([dense_down, swap(dense_down)], axis=0)
    mix_pair = jnp.concatenate([dense_mix, swap(dense_mix)], axis=0)

    wide = all_tokens.astype(F32)
    mean_in = jnp.mean(wide * wide, axis=-1, keepdims=True) * (1.0 / TOKEN_SCALE**2)
    row_scale = lax.rsqrt(mean_in + EPS) * (1.0 / TOKEN_SCALE)
    gained = (gain_in[:, None] * proj_in.astype(F32)).astype(BF16)
    units = jnp.dot(all_tokens, gained, preferred_element_type=F32) * row_scale
    branch, new_real, new_imag = state_step(
        units.astype(BF16),
        state_real,
        state_imag,
        decay_rate,
        frequency,
        log_step,
        input_real,
        input_imag,
        output_real,
        output_imag,
        skip_gain,
    )
    by_core = (branch * BRANCH_SCALE).astype(F16).T.reshape(-1, chips, cores, rows)

    def half_of(index):
        return lax.dynamic_index_in_dim(by_core, index, 2, keepdims=False).reshape(-1, half)

    kept, got = half_of(core), swap(half_of(1 - core))
    both = jnp.where(
        core == 0, jnp.concatenate([kept, got], axis=0), jnp.concatenate([got, kept], axis=0)
    )
    lanes = jnp.arange(half)
    routing_rows = jnp.where(lanes // rows == chip, jnp.tile(routing.T, (1, chips)), 0.0)
    routing_rows = jnp.pad(routing_rows.astype(F16), ((0, 16 - 3 * top_count), (0, 0)))
    branch_and_routing = lax.all_gather(
        jnp.concatenate([both, routing_rows], axis=0), "chip", axis=0, tiled=False
    )
    channels = both.shape[0]
    all_branch = branch_and_routing[:, :channels].reshape(-1, half).astype(BF16)
    mixed, own_residual = mixer(
        jnp.stack([chip, core]),
        all_branch,
        all_proj,
        all_tokens.reshape(chips, cores, rows, width),
        gain_mid,
    )

    products = lax.dot_general(
        dense_pair, mixed, (((1,), (1,)), ((), ())), preferred_element_type=F32
    ).reshape(cores, 2, -1, half)
    hidden = (jax.nn.silu(products[:, 0]) * products[:, 1]).astype(BF16).reshape(-1, half)
    logit_term = jnp.sum(hidden.astype(F32) * mix_pair[:, None], axis=0)
    logit_terms = lax.all_to_all(
        jnp.broadcast_to(logit_term[None], (chips, half)), "chip", 0, 0, tiled=True
    )

    table = jnp.sum(branch_and_routing[:, channels : channels + 3 * top_count].astype(F32), axis=0)
    names = table[:top_count]
    weights = (table[top_count : 2 * top_count] + table[2 * top_count :]) * (1.0 / SHARE_SCALE)
    before = (
        (lanes[:, None] < lanes[None, :]) & (lanes[:, None] // rows == lanes[None, :] // rows)
    ).astype(BF16)
    first = (lanes // rows * capacity).astype(F32)[None, :]
    slot_ids = jnp.arange(slots).astype(F32)[:, None]

    def slot_table(expert):
        hit = names == expert.astype(F32)
        share = jnp.sum(jnp.where(hit, weights, 0.0), axis=0, keepdims=True)
        marked = jnp.any(hit, axis=0, keepdims=True)
        rank = jnp.dot(marked.astype(BF16), before, preferred_element_type=F32)
        chosen = jnp.where(marked, first + rank, -1.0) == slot_ids
        return (chosen, jnp.sum(jnp.where(chosen, share, 0.0), axis=1, keepdims=True))

    own_chosen, own_share = slot_table(chip * cores + core)
    pair_chosen, pair_share = slot_table(chip * cores + (1 - core))
    selector = jnp.concatenate([own_chosen, pair_chosen], axis=0).astype(BF16)
    slot_share = jnp.concatenate([own_share, pair_share], axis=0)
    picked = jnp.dot(selector, mixed, preferred_element_type=F32).astype(BF16)
    picked = jnp.concatenate([picked[:slots], swap(picked[slots:])], axis=0)
    result = expert_apply(picked, expert_gate, expert_up, expert_down)
    result = jnp.concatenate([result[:slots], swap(result[slots:])], axis=0)
    result = (result.astype(F32) * slot_share).astype(BF16)

    gate_weight = jax.nn.sigmoid(jnp.sum(logit_terms, axis=0, keepdims=True))
    gated_hidden = (gate_weight * hidden.astype(F32)).astype(BF16)
    combined = lax.dot_general(
        jnp.concatenate([gated_hidden, selector], axis=0),
        jnp.concatenate([down_pair, result], axis=0),
        (((0,), (0,)), ((), ())),
        preferred_element_type=F32,
    ).astype(BF16)
    parts = combined.reshape(chips, rows, width)
    summed = jnp.concatenate(
        [reduce_to_own(part) for part in jnp.split(parts, REDUCE_PARTS, axis=2)], axis=1
    )
    layer_out = (own_residual + summed).astype(BF16)
    return (layer_out, new_real, new_imag)


def solution(mesh):
    cores = 2
    split = Mesh(
        mesh.devices.reshape(mesh.shape["grp"], mesh.shape["ep"] // cores, cores),
        ("grp", "chip", "core"),
    )
    return jax.shard_map(
        on_device,
        mesh=split,
        in_specs=(
            P(GRP_EP, None),
            P(GRP_EP, None),
            P(GRP_EP, None),
            P("grp", EP, None),
            P("grp", EP, None),
            P(),
            P(None, EP),
            P(EP, None),
            P(EP, None),
            P(EP),
            P(EP, None, None),
            P(EP, None, None),
            P(EP, None, None),
            P(EP, None, None),
            P(EP, None),
            P(EP, None),
            P(),
            P(EP, None, None),
            P(EP, None, None),
            P(EP, None, None),
            P(None, EP),
            P(None, EP),
            P(EP, None),
            P(EP),
        ),
        out_specs=(P(GRP_EP, None), P("grp", EP, None), P("grp", EP, None)),
        check_vma=False,
    )
```

```python
import jax
import jax.numpy as jnp
from jax import lax
from jax.experimental import pallas as pl
from jax.experimental.pallas import tpu as pltpu
from jax.sharding import Mesh
from jax.sharding import PartitionSpec as P

EP = ("chip", "core")
GRP_EP = ("grp", "chip", "core")

EPS = 1e-06
LIMIT = 7.0
ALPHA = 1.702

TOKEN_SCALE = 2.0**12
BRANCH_SCALE = 2.0**-4
PROJ_SCALE = TOKEN_SCALE / BRANCH_SCALE
SHARE_SCALE = 2.0**12

MIXER_STEPS = 2
EXPERT_STEPS = 2
REDUCE_PARTS = 2

F32 = jnp.float32
BF16 = jnp.bfloat16
F16 = jnp.float16


def state_step(
    inputs,
    state_real,
    state_imag,
    decay_rate,
    frequency,
    log_step,
    input_real,
    input_imag,
    output_real,
    output_imag,
    skip_gain,
):
    seq_count = inputs.shape[0]
    groups, group_size = skip_gain.shape
    inputs = inputs.astype(F32).reshape(seq_count, groups, group_size)
    step_size = jnp.exp(log_step)[:, None]
    decay_part = -decay_rate
    magnitude = jnp.exp(decay_part * step_size)
    carry_real = magnitude * jnp.cos(frequency * step_size)
    carry_imag = magnitude * jnp.sin(frequency * step_size)
    denom = decay_part * decay_part + frequency * frequency
    feed_real = ((carry_real - 1.0) * decay_part + carry_imag * frequency) / denom
    feed_imag = (carry_imag * decay_part - (carry_real - 1.0) * frequency) / denom
    drive_real = jnp.einsum("sgp,gnp->sgn", inputs, input_real)
    drive_imag = jnp.einsum("sgp,gnp->sgn", inputs, input_imag)
    new_real = (
        carry_real * state_real
        - carry_imag * state_imag
        + feed_real * drive_real
        - feed_imag * drive_imag
    )
    new_imag = (
        carry_real * state_imag
        + carry_imag * state_real
        + feed_real * drive_imag
        + feed_imag * drive_real
    )
    readout = (
        jnp.einsum("gpn,sgn->sgp", output_real, new_real)
        - jnp.einsum("gpn,sgn->sgp", output_imag, new_imag)
        + skip_gain * inputs
    )
    branch = jax.nn.gelu(readout).reshape(seq_count, groups * group_size)
    return (branch, new_real, new_imag)


def swap(x):
    return lax.ppermute(x, "core", [(0, 1), (1, 0)])


def reduce_to_own(blocks):
    chips = blocks.shape[0]
    cores = lax.axis_size("core")
    chip = lax.axis_index("chip")
    core = lax.axis_index("core")
    span = (chips - 1) // 3
    reach = span // 2
    assert chips == 3 * (2 * reach + 1) + 1

    def part(k):
        return lax.dynamic_index_in_dim(blocks, (chip + k) % chips, 0, keepdims=False).astype(F32)

    def send(x, hops):
        pairs = [(i, (i + hops) % chips) for i in range(chips)]
        return lax.ppermute(x.astype(BF16), "chip", pairs).astype(F32)

    def send_both_ways(x, hops):
        pairs = [
            (i * cores + c, (i + (hops if c == 0 else -hops)) % chips * cores + c)
            for i in range(chips)
            for c in range(cores)
        ]
        return lax.ppermute(x.astype(BF16), ("chip", "core"), pairs).astype(F32)

    far = chips // 2
    up = jnp.stack([part(span + reach), part(reach - span), part(reach)])
    down = jnp.stack([part(-span - reach), part(span - reach), part(-reach)])
    left_over = send_both_ways(part(far), far - (span + reach - 1))
    for s in range(reach - 1, -1, -1):
        up, down = send(up, 1), send(down, -1)
        if s > 0:
            up = up + jnp.stack([part(span + s), part(s - span), part(s)])
            down = down + jnp.stack([part(-span - s), part(span - s), part(-s)])
        if s == reach - 1:
            up = up.at[0].add(jnp.where(core == 0, left_over, 0.0))
            down = down.at[0].add(jnp.where(core == 0, 0.0, left_over))
    from_below = send(part(span) + up[0] + down[1], span)
    from_above = send(part(-span) + up[1] + down[0], -span)
    return part(0) + up[2] + down[2] + from_below + from_above


def mixer_kernel(place, branch, proj, tokens, gain, mixed, own, total):
    rows, block = own.shape[0], total.shape[0]
    total[...] = (
        tokens[...].reshape(total.shape).astype(F32)
        + lax.dot_general(
            branch[...], proj[...], (((0,), (0,)), ((), ())), preferred_element_type=F32
        )
    ) * (1.0 / TOKEN_SCALE)
    values = total[...]
    mean = jnp.mean(values * values, axis=-1, keepdims=True)
    mixed[...] = (values * lax.rsqrt(mean + EPS) * gain[...]).astype(BF16)
    at = place[0] * rows

    @pl.when(at // block == pl.program_id(0))
    def _():
        own[...] = total[pl.ds(pl.multiple_of(at % block, rows), rows), :]


def mixer(place, branch, proj, tokens, gain):
    chips, _, rows, width = tokens.shape
    held = chips // MIXER_STEPS
    whole = lambda i, place: (0, 0)
    return pl.pallas_call(
        mixer_kernel,
        grid_spec=pltpu.PrefetchScalarGridSpec(
            num_scalar_prefetch=1,
            grid=(MIXER_STEPS,),
            in_specs=[
                pl.BlockSpec((branch.shape[0], held * rows), lambda i, place: (0, i)),
                pl.BlockSpec(proj.shape, whole),
                pl.BlockSpec((held, 1, rows, width), lambda i, place: (i, place[1], 0, 0)),
                pl.BlockSpec((1, width), whole),
            ],
            out_specs=[
                pl.BlockSpec((held * rows, width), lambda i, place: (i, 0)),
                pl.BlockSpec((rows, width), whole),
            ],
            scratch_shapes=[pltpu.VMEM((held * rows, width), F32)],
        ),
        out_shape=[
            jax.ShapeDtypeStruct((chips * rows, width), BF16),
            jax.ShapeDtypeStruct((rows, width), F32),
        ],
        compiler_params=pltpu.CompilerParams(vmem_limit_bytes=48 * 2**20),
        name="mixer",
    )(place, branch, proj, tokens, gain.reshape(1, width))


def expert_kernel(picked, gate, up, down, result, total):
    gated = jnp.minimum(jnp.dot(picked[...], gate[0], preferred_element_type=F32), LIMIT)
    upper = jnp.clip(jnp.dot(picked[...], up[0], preferred_element_type=F32), -LIMIT, LIMIT)
    activated = ((upper + 1.0) * gated * jax.nn.sigmoid(ALPHA * gated)).astype(BF16)
    part = jnp.dot(activated, down[0], preferred_element_type=F32)

    @pl.when(pl.program_id(0) == 0)
    def _():
        total[...] = part

    @pl.when(pl.program_id(0) > 0)
    def _():
        total[...] += part

    @pl.when(pl.program_id(0) == pl.num_programs(0) - 1)
    def _():
        result[...] = total[...].astype(BF16)


def expert_apply(picked, gate, up, down):
    count, width = picked.shape
    hidden = gate.shape[2]
    block = hidden // EXPERT_STEPS
    return pl.pallas_call(
        expert_kernel,
        grid=(hidden // block,),
        in_specs=[
            pl.BlockSpec((count, width), lambda i: (0, 0)),
            pl.BlockSpec((1, width, block), lambda i: (0, 0, i)),
            pl.BlockSpec((1, width, block), lambda i: (0, 0, i)),
            pl.BlockSpec((1, block, width), lambda i: (0, i, 0)),
        ],
        out_specs=pl.BlockSpec((count, width), lambda i: (0, 0)),
        out_shape=jax.ShapeDtypeStruct((count, width), BF16),
        scratch_shapes=[pltpu.VMEM((count, width), F32)],
        compiler_params=pltpu.CompilerParams(vmem_limit_bytes=48 * 2**20),
        name="expert",
    )(picked, gate, up, down)


def on_device(
    tokens,
    routes,
    route_logits,
    state_real,
    state_imag,
    gain_in,
    proj_in,
    decay_rate,
    frequency,
    log_step,
    input_real,
    input_imag,
    output_real,
    output_imag,
    skip_gain,
    proj_out,
    gain_mid,
    expert_gate,
    expert_up,
    expert_down,
    dense_gate,
    dense_up,
    dense_down,
    dense_mix,
):
    chips = lax.axis_size("chip")
    cores = lax.axis_size("core")
    devices = chips * cores
    chip = lax.axis_index("chip")
    core = lax.axis_index("core")
    rows, width = tokens.shape
    top_count = routes.shape[1]
    capacity = max(2, 2 * rows * top_count // devices)
    half = chips * rows
    slots = chips * capacity

    shares = jnp.exp(route_logits)
    shares = shares / jnp.sum(shares, axis=1, keepdims=True) * SHARE_SCALE
    shares_high = shares.astype(F16)
    shares_low = (shares - shares_high.astype(F32)).astype(F16)
    routing = jnp.concatenate([routes.astype(F16), shares_high, shares_low], axis=1)
    sent = jnp.stack(
        [
            (tokens.astype(F32) * TOKEN_SCALE).astype(F16),
            (proj_out.astype(F32) * PROJ_SCALE).astype(F16),
        ]
    )
    gathered = lax.all_gather(sent, EP, axis=0, tiled=False)
    all_tokens, all_proj = lax.optimization_barrier(
        (
            gathered[:, 0].reshape(-1, width).astype(BF16),
            gathered[:, 1].reshape(-1, width).astype(BF16),
        )
    )
    own_dense = jnp.concatenate([dense_gate.T, dense_up.T, dense_down], axis=0)
    pair_dense = swap(own_dense)
    into = 2 * dense_gate.shape[1]
    dense_pair = jnp.concatenate([own_dense[:into], pair_dense[:into]], axis=0)
    down_pair = jnp.concatenate([own_dense[into:], pair_dense[into:]], axis=0)
    mix_pair = jnp.concatenate([dense_mix, swap(dense_mix)], axis=0)

    wide = all_tokens.astype(F32)
    mean_in = jnp.mean(wide * wide, axis=-1, keepdims=True) * (1.0 / TOKEN_SCALE**2)
    row_scale = lax.rsqrt(mean_in + EPS) * (1.0 / TOKEN_SCALE)
    gained = (gain_in[:, None] * proj_in.astype(F32)).astype(BF16)
    units = jnp.dot(all_tokens, gained, preferred_element_type=F32) * row_scale
    branch, new_real, new_imag = state_step(
        units.astype(BF16),
        state_real,
        state_imag,
        decay_rate,
        frequency,
        log_step,
        input_real,
        input_imag,
        output_real,
        output_imag,
        skip_gain,
    )
    by_core = (branch * BRANCH_SCALE).astype(F16).T.reshape(-1, chips, cores, rows)

    def half_of(index):
        return lax.dynamic_index_in_dim(by_core, index, 2, keepdims=False).reshape(-1, half)

    kept, got = half_of(core), swap(half_of(1 - core))
    both = jnp.where(
        core == 0, jnp.concatenate([kept, got], axis=0), jnp.concatenate([got, kept], axis=0)
    )
    lanes = jnp.arange(half)
    routing_rows = jnp.where(lanes // rows == chip, jnp.tile(routing.T, (1, chips)), 0.0)
    routing_rows = jnp.pad(routing_rows.astype(F16), ((0, 16 - 3 * top_count), (0, 0)))
    branch_and_routing = lax.all_gather(
        jnp.concatenate([both, routing_rows], axis=0), "chip", axis=0, tiled=False
    )
    channels = both.shape[0]
    all_branch = branch_and_routing[:, :channels].reshape(-1, half).astype(BF16)
    mixed, own_residual = mixer(
        jnp.stack([chip, core]),
        all_branch,
        all_proj,
        all_tokens.reshape(chips, cores, rows, width),
        gain_mid,
    )

    products = lax.dot_general(
        dense_pair, mixed, (((1,), (1,)), ((), ())), preferred_element_type=F32
    ).reshape(cores, 2, -1, half)
    hidden = (jax.nn.silu(products[:, 0]) * products[:, 1]).astype(BF16).reshape(-1, half)
    logit_term = jnp.sum(hidden.astype(F32) * mix_pair[:, None], axis=0)
    logit_terms = lax.all_to_all(
        jnp.broadcast_to(logit_term[None], (chips, half)), "chip", 0, 0, tiled=True
    )

    table = jnp.sum(branch_and_routing[:, channels : channels + 3 * top_count].astype(F32), axis=0)
    names = table[:top_count]
    weights = (table[top_count : 2 * top_count] + table[2 * top_count :]) * (1.0 / SHARE_SCALE)
    before = (
        (lanes[:, None] < lanes[None, :]) & (lanes[:, None] // rows == lanes[None, :] // rows)
    ).astype(BF16)
    first = (lanes // rows * capacity).astype(F32)[None, :]
    slot_ids = jnp.arange(slots).astype(F32)[:, None]

    def slot_table(expert):
        hit = names == expert.astype(F32)
        share = jnp.sum(jnp.where(hit, weights, 0.0), axis=0, keepdims=True)
        marked = jnp.any(hit, axis=0, keepdims=True)
        rank = jnp.dot(marked.astype(BF16), before, preferred_element_type=F32)
        chosen = jnp.where(marked, first + rank, -1.0) == slot_ids
        return (chosen, jnp.sum(jnp.where(chosen, share, 0.0), axis=1, keepdims=True))

    own_chosen, own_share = slot_table(chip * cores + core)
    pair_chosen, pair_share = slot_table(chip * cores + (1 - core))
    selector = jnp.concatenate([own_chosen, pair_chosen], axis=0).astype(BF16)
    slot_share = jnp.concatenate([own_share, pair_share], axis=0)
    picked = jnp.dot(selector, mixed, preferred_element_type=F32).astype(BF16)
    picked = jnp.concatenate([picked[:slots], swap(picked[slots:])], axis=0)
    result = expert_apply(picked, expert_gate, expert_up, expert_down)
    result = jnp.concatenate([result[:slots], swap(result[slots:])], axis=0)
    result = (result.astype(F32) * slot_share).astype(BF16)

    gate_weight = jax.nn.sigmoid(jnp.sum(logit_terms, axis=0, keepdims=True))
    gated_hidden = (gate_weight * hidden.astype(F32)).astype(BF16)
    combined = lax.dot_general(
        jnp.concatenate([gated_hidden, selector], axis=0),
        jnp.concatenate([down_pair, result], axis=0),
        (((0,), (0,)), ((), ())),
        preferred_element_type=F32,
    ).astype(BF16)
    parts = combined.reshape(chips, rows, width)
    summed = jnp.concatenate(
        [reduce_to_own(part) for part in jnp.split(parts, REDUCE_PARTS, axis=2)], axis=1
    )
    layer_out = (own_residual + summed).astype(BF16)
    return (layer_out, new_real, new_imag)


def solution(mesh):
    cores = 2
    split = Mesh(
        mesh.devices.reshape(mesh.shape["grp"], mesh.shape["ep"] // cores, cores),
        ("grp", "chip", "core"),
    )
    return jax.shard_map(
        on_device,
        mesh=split,
        in_specs=(
            P(GRP_EP, None),
            P(GRP_EP, None),
            P(GRP_EP, None),
            P("grp", EP, None),
            P("grp", EP, None),
            P(),
            P(None, EP),
            P(EP, None),
            P(EP, None),
            P(EP),
            P(EP, None, None),
            P(EP, None, None),
            P(EP, None, None),
            P(EP, None, None),
            P(EP, None),
            P(EP, None),
            P(),
            P(EP, None, None),
            P(EP, None, None),
            P(EP, None, None),
            P(None, EP),
            P(None, EP),
            P(EP, None),
            P(EP),
        ),
        out_specs=(P(GRP_EP, None), P("grp", EP, None), P("grp", EP, None)),
        check_vma=False,
    )
```
